512 devices in a mesh: sp: 64 (over z, y), tp: 8 (over x, core).
Axes of the slice: x: 4, y: 4, z: 16, core: 2. Of those that a mesh axis runs over, the one named last changes fastest.
Arguments:
- layer_input_sequence: bfloat16 [24576, 2048], P('sp', 'tp'), may hold values from -6 to 6
- probe_projection_matrix: bfloat16 [2048, 1024], P(None, 'tp'), may hold values from -0.125 to 0.125
- address_projection_matrix: bfloat16 [2048, 1024], P(None, 'tp'), may hold values from -0.125 to 0.125
- content_projection_matrix: bfloat16 [2048, 1024], P(None, 'tp'), may hold values from -2 to 2
- result_valve_matrix: bfloat16 [2048, 1024], P(None, 'tp'), may hold values from -0.125 to 0.125
- shrink_strength_matrix: bfloat16 [2, 2048, 8], replicated, may hold values from -0.125 to 0.125
- causal_filter_coefficients: bfloat16 [3, 4, 1024], P(None, None, 'tp'), may hold values from -3 to 3
- channel_group_fading_speed: float32 [8], replicated, may hold values from 0 to 0.06, as said below
- summed_shrink_logs: float32 [24576, 8], P('sp', 'tp'), may hold values from -0.7 to 0, as said below
- result_scaling_vector: bfloat16 [128], replicated, may hold values from 0.099609375 to 1.8984375
- generated_probe_vector: bfloat16 [64, 8, 128], P('sp', 'tp'), may hold values from -6 to 6
Outputs:
- mixed: bfloat16 [24576, 1024], P('sp', 'tp')
- cache: bfloat16 [8, 128, 128], P('tp')
- new_read: float32 [64, 8, 128], P('sp', 'tp')
The draws below stay inside these ranges and needn't reach their ends.
Inputs may be any that keep to these rules, and one draw needn't show every extreme that they name: `channel_group_fading_speed`: positive rates of each head. `summed_shrink_logs`: zero at all but a few positions of each head.
All inputs are finite; a program needn't handle non-finite values.
Results may differ from the reference program's by a relative error of at most 0.0095.
Values may be sent and summed in bfloat16 or wider, within the bound.
A program may use at most 64 MiB of HBM per device.

```python
import math
import jax
import jax.numpy as jnp
from jax import lax

D = 2048
H = 8
DK = 128
BLK = 64
CONV = 4
SEQ = 24576
N_SP = 64


def draw_channel_group_fading_speed(key, part):
    fast_key, pick_key, slow_key = jax.random.split(jax.random.fold_in(key, 11), 3)
    fast = jnp.exp(jax.random.uniform(fast_key, (H,), jnp.float32, math.log(0.025), math.log(0.06)))
    slow = jnp.exp(jax.random.uniform(slow_key, (H,), jnp.float32, math.log(0.2), math.log(1.0))) / SEQ
    share = 0.5
    chosen = jax.random.uniform(pick_key, (H,), jnp.float32) < share
    return jnp.where(chosen, fast, slow)


def draw_summed_shrink_logs(key, part):
    where_key, size_key = jax.random.split(jax.random.fold_in(key, 23), 2)
    quarter = SEQ // 4
    spots = jnp.arange(4)[:, None] * quarter + jax.random.randint(where_key, (4, H), 0, quarter)
    depth = jnp.log(jax.random.uniform(size_key, (4, H), jnp.float32, 0.5, 0.8))
    position = jnp.arange(SEQ)[:, None, None]
    return jnp.sum(jnp.where(position == spots[None], depth[None], 0.0), axis=1)


def levels(key, dims, cuts, low, high):
    def one(axis_at, shards_of):
        heights = jax.random.uniform(jax.random.fold_in(jax.random.fold_in(key, 6), axis_at), (shards_of,), jnp.float32, low / len(cuts), high / len(cuts))
        return jnp.repeat(jnp.exp(heights), dims[axis_at] // shards_of).reshape((-1,) + (1,) * (len(dims) - axis_at - 1))

    factor_of = one(*cuts[0])
    for cut in cuts[1:]:
        factor_of = factor_of * one(*cut)
    return factor_of


def noise(key, shape, scale, limit, pieces=(), kind=jnp.bfloat16):
    entries = scale * jax.random.normal(key, shape, jnp.float32)
    if pieces:
        entries = entries * levels(key, shape, pieces, -0.22, 0.18)
    return jnp.clip(entries, -limit, limit).astype(kind)


def setup_inputs(seed: int = 0) -> dict:
    key_list = jax.random.split(jax.random.key(seed), 12)
    return {
        "layer_input_sequence": noise(key_list[0], (SEQ, D), 1.0, 6.0, ((0, 64), (1, 8))),
        "probe_projection_matrix": noise(key_list[1], (D, H * DK), D ** -0.5, 0.125, ((1, 8),)),
        "address_projection_matrix": noise(key_list[2], (D, H * DK), D ** -0.5, 0.125, ((1, 8),)),
        "content_projection_matrix": noise(key_list[3], (D, H * DK), (max(1, D * DK // SEQ)) ** -0.5, 2.0, ((1, 8),)),
        "result_valve_matrix": noise(key_list[4], (D, H * DK), D ** -0.5, 0.125, ((1, 8),)),
        "shrink_strength_matrix": noise(key_list[5], (2, D, H), D ** -0.5, 0.125),
        "causal_filter_coefficients": noise(key_list[6], (3, CONV, H * DK), 0.5, 3.0, ((2, 8),)),
        "channel_group_fading_speed": draw_channel_group_fading_speed(jax.random.fold_in(key_list[11], 71), 0),
        "summed_shrink_logs": draw_summed_shrink_logs(jax.random.fold_in(key_list[11], 71), 0),
        "result_scaling_vector": jnp.clip(1.0 + 0.18 * jax.random.normal(key_list[9], (DK,), jnp.float32), 0.099609375, 1.8984375).astype(jnp.bfloat16),
        "generated_probe_vector": noise(key_list[10], (N_SP, H, DK), 1.0, 6.0, ((0, 64), (1, 8))),
    }


EPS = 1e-06
HIGH = lax.Precision.HIGHEST

def silu(value):
    return value * jax.nn.sigmoid(value)

def l2_unit(value):
    return value * lax.rsqrt(lax.optimization_barrier(jnp.sum(value * value, axis=-1, keepdims=True)) + EPS)

def causal_mix(raw, taps):
    length = raw.shape[0]
    padded = jnp.pad(raw.astype(jnp.float32), ((CONV - 1, 0), (0, 0)))
    total = jnp.zeros((length, raw.shape[1]), jnp.float32)
    for lag in range(CONV):
        total = total + taps[lag].astype(jnp.float32) * padded[lag:lag + length]
    return silu(total)

def block_terms(query, keys, values, fading_exponent, beta):
    heads, length, width = keys.shape
    count = length // BLK

    def split(array):
        return array.reshape((heads, count, BLK) + array.shape[2:])
    query, keys, values, fading_exponent, beta = (split(a) for a in (query, keys, values, fading_exponent, beta))
    summed = jnp.cumsum(fading_exponent, axis=-1)
    places = jnp.arange(BLK)
    inclusive = places[:, None] >= places[None, :]
    strict = places[:, None] > places[None, :]
    decay = jnp.exp(jnp.where(inclusive, summed[..., :, None] - summed[..., None, :], -1e+30))
    k_beta = keys * beta[..., None]
    a_mat = jnp.where(strict, jnp.einsum('hncd,hnsd->hncs', k_beta, keys, precision=HIGH) * decay, 0.0)
    eye = jnp.eye(BLK, dtype=jnp.float32)
    t_mat = lax.linalg.triangular_solve(eye + a_mat, jnp.broadcast_to(eye, a_mat.shape), left_side=True, lower=True, unit_diagonal=True)
    u_part = jnp.einsum('hncs,hnsd->hncd', t_mat, values * beta[..., None], precision=HIGH)
    w_part = jnp.einsum('hncs,hnsd->hncd', t_mat, k_beta * jnp.exp(summed)[..., None], precision=HIGH)
    attend = jnp.where(inclusive, jnp.einsum('hncd,hnsd->hncs', query, keys, precision=HIGH) * decay, 0.0)
    q_dec = query * jnp.exp(summed)[..., None]
    k_dec = keys * jnp.exp(summed[..., -1:] - summed)[..., None]
    g_last = jnp.exp(summed[..., -1])
    return (u_part, w_part, q_dec, k_dec, attend, g_last)

def reference(layer_input_sequence, probe_projection_matrix, address_projection_matrix, content_projection_matrix, result_valve_matrix, shrink_strength_matrix, causal_filter_coefficients, channel_group_fading_speed, summed_shrink_logs, result_scaling_vector, generated_probe_vector):
    length = layer_input_sequence.shape[0]

    def project(weight):
        return jnp.dot(layer_input_sequence.astype(jnp.float32), weight.astype(jnp.float32), preferred_element_type=jnp.float32).astype(jnp.bfloat16)
    q_raw, k_raw, v_raw, z_raw = (project(w) for w in (probe_projection_matrix, address_projection_matrix, content_projection_matrix, result_valve_matrix))
    speed_entries = jnp.einsum('sd,rdh->srh', layer_input_sequence.astype(jnp.float32), shrink_strength_matrix.astype(jnp.float32), precision=HIGH)
    query = l2_unit(causal_mix(q_raw, causal_filter_coefficients[0]).reshape(length, H, DK)) * DK ** (-0.5)
    keys = l2_unit(causal_mix(k_raw, causal_filter_coefficients[1]).reshape(length, H, DK))
    values = causal_mix(v_raw, causal_filter_coefficients[2]).reshape(length, H, DK)
    write_shift = math.log(4.0 * length / DK)
    beta = jax.nn.sigmoid(speed_entries[:, 1, :] - write_shift)
    fading_exponent = -channel_group_fading_speed[None, :] * jax.nn.softplus(speed_entries[:, 0, :]) + summed_shrink_logs
    terms = block_terms(query.transpose(1, 0, 2), keys.transpose(1, 0, 2), values.transpose(1, 0, 2), fading_exponent.T, beta.T)

    def advance(state, inputs):
        u_i, w_i, qd_i, kd_i, a_i, gl_i = inputs
        v_new = u_i - jnp.einsum('hcd,hde->hce', w_i, state, precision=HIGH)
        out_i = jnp.einsum('hcd,hde->hce', qd_i, state, precision=HIGH) + jnp.einsum('hcs,hse->hce', a_i, v_new, precision=HIGH)
        state = state * gl_i[:, None, None] + jnp.einsum('hcd,hce->hde', kd_i, v_new, precision=HIGH)
        return (state, out_i)
    inputs = tuple((jnp.moveaxis(t, 1, 0) for t in terms))
    state, outs = lax.scan(advance, jnp.zeros((H, DK, DK), jnp.float32), inputs)
    heads_out = outs.transpose(1, 0, 2, 3).reshape(H, length, DK).transpose(1, 0, 2)
    normed = heads_out * lax.rsqrt(lax.optimization_barrier(jnp.mean(heads_out * heads_out, axis=-1, keepdims=True)) + EPS)
    gated = normed * result_scaling_vector.astype(jnp.float32) * silu(z_raw.reshape(length, H, DK).astype(jnp.float32))
    mixed = gated.reshape(length, H * DK).astype(jnp.bfloat16)
    cache = state.astype(jnp.bfloat16)
    unit_query = l2_unit(generated_probe_vector.astype(jnp.float32)) * DK ** (-0.5)
    new_read = jnp.einsum('nhd,hde->nhe', unit_query, cache.astype(jnp.float32), precision=HIGH)
    return (mixed, cache, new_read)
```

```python
import functools
import math

import jax
import jax.numpy as jnp
from jax import lax
from jax.experimental import pallas as pl
from jax.experimental.pallas import tpu as pltpu
from jax.sharding import PartitionSpec as P

DK = 128
CONV = 4
EPS = 1e-06
MESH = pl.DeviceIdType.MESH
F32 = jnp.float32
BF16 = jnp.bfloat16

ROWS = 128
RIM = 16


def silu(value):
    return value * jax.nn.sigmoid(value)


def halves(value):
    high = value.astype(BF16)
    low = (value - high.astype(F32)).astype(BF16)
    return high, low


def dot(left, right, dims):
    return lax.dot_general(left, right, dims, preferred_element_type=F32)


def dot3(left, right, dims):
    lh, ll = halves(left)
    rh, rl = halves(right)
    return dot(lh, rh, dims) + (dot(lh, rl, dims) + dot(ll, rh, dims))


NN = (((1,), (0,)), ((), ()))
TN = (((0,), (0,)), ((), ()))
BNN = (((2,), (1,)), ((0,), (0,)))
BNT = (((2,), (2,)), ((0,), (0,)))


def project_kernel(
    x_hbm, wq_hbm, wk_hbm, wv_hbm, wz_hbm, wr_hbm,
    raw_ref, rates_ref, rim_ref,
    x_all, w_all, w_rate, tail, rim_in,
    load_sem, send_sem, recv_sem, pass_sem, got_sem, rim_sem,
):
    sp = lax.axis_index("sp")
    tp = lax.axis_index("tp")
    n_sp = lax.axis_size("sp")
    chip, core = tp // 2, tp % 2
    partner = chip * 2 + (1 - core)
    rows, width = x_hbm.shape
    parts = rows // ROWS

    def columns(slot):
        return pl.ds(pl.multiple_of(slot * width, width), width)

    load_x = pltpu.make_async_copy(x_hbm, x_all.at[:, columns(tp)], load_sem.at[0])
    load_x.start()
    loads = []
    for i, w in enumerate((wq_hbm, wk_hbm, wv_hbm, wz_hbm)):
        loads.append(
            pltpu.make_async_copy(w, w_all.at[:, pl.ds(i * DK, DK)], load_sem.at[1 + i])
        )
    loads.append(pltpu.make_async_copy(wr_hbm, w_rate, load_sem.at[5]))
    for load in loads:
        load.start()

    after, before = (sp + 1) % n_sp, (sp + n_sp - 1) % n_sp
    barrier = pltpu.get_barrier_semaphore()
    for r in (2, 1, 3):
        peer = ((chip + r) % 4) * 2 + core
        pl.semaphore_signal(barrier, inc=1, device_id=(sp, peer), device_id_type=MESH)
    pl.semaphore_signal(barrier, inc=1, device_id=(sp, partner), device_id_type=MESH)
    pl.semaphore_signal(barrier, inc=1, device_id=(after, tp), device_id_type=MESH)
    pl.semaphore_signal(barrier, inc=1, device_id=(before, tp), device_id_type=MESH)
    load_x.wait()
    pl.semaphore_wait(barrier, 6)

    order = [parts - 1] + list(range(parts - 1))
    sends = {}

    def block(part, slot):
        return x_all.at[pl.ds(part * ROWS, ROWS), columns(slot)]

    for part in order:
        for r in (1, 3, 2):
            peer = ((chip + r) % 4) * 2 + core
            copy = pltpu.make_async_remote_copy(
                src_ref=block(part, tp), dst_ref=block(part, tp),
                send_sem=send_sem.at[part, r], recv_sem=recv_sem.at[part, r],
                device_id=(sp, peer), device_id_type=MESH,
            )
            copy.start()
            sends[part, r] = copy
        copy = pltpu.make_async_remote_copy(
            src_ref=block(part, tp), dst_ref=block(part, tp),
            send_sem=pass_sem.at[part, 0], recv_sem=got_sem.at[part, 0],
            device_id=(sp, partner), device_id_type=MESH,
        )
        copy.start()
        sends[part, 0] = copy

    for load in loads:
        load.wait()

    passes = []
    rim_copy = None
    for part in order:
        for r in (1, 3, 2):
            sends[part, r].wait_recv()
            slot = ((chip + 4 - r) % 4) * 2 + core
            copy = pltpu.make_async_remote_copy(
                src_ref=block(part, slot), dst_ref=block(part, slot),
                send_sem=pass_sem.at[part, r], recv_sem=got_sem.at[part, r],
                device_id=(sp, partner), device_id_type=MESH,
            )
            copy.start()
            passes.append(copy)
        sends[part, 0].wait_recv()
        for copy in passes[-3:]:
            copy.wait_recv()
        x = x_all[pl.ds(part * ROWS, ROWS), :]
        here = pl.ds(part * ROWS, ROWS)
        raw = dot(x, w_all[...], NN).astype(BF16)
        raw_ref[here, :] = raw
        if rim_copy is None:
            tail[...] = raw[ROWS - RIM :, : 3 * DK]
        rates_ref[0, here, :] = dot(x, w_rate[0], NN)
        rates_ref[1, here, :] = dot(x, w_rate[1], NN)
        if rim_copy is None:
            rim_copy = pltpu.make_async_remote_copy(
                src_ref=tail, dst_ref=rim_in,
                send_sem=rim_sem.at[0], recv_sem=rim_sem.at[1],
                device_id=(after, tp), device_id_type=MESH,
            )
            rim_copy.start()
    rim_copy.wait_recv()
    rim_ref[...] = rim_in[...]
    rim_copy.wait_send()
    for copy in sends.values():
        copy.wait_send()
    for copy in passes:
        copy.wait_send()


def project(x, wq, wk, wv, wz, wr):
    rows, width = x.shape
    depth = wq.shape[0]
    parts = rows // ROWS
    heads = wr.shape[2]
    any_space = pl.BlockSpec(memory_space=pl.ANY)
    vmem = pl.BlockSpec(memory_space=pltpu.VMEM)
    return pl.pallas_call(
        project_kernel,
        out_shape=(
            jax.ShapeDtypeStruct((rows, 4 * DK), BF16),
            jax.ShapeDtypeStruct((2, rows, heads), F32),
            jax.ShapeDtypeStruct((RIM, 3 * DK), BF16),
        ),
        in_specs=[any_space] * 6,
        out_specs=(vmem, vmem, vmem),
        scratch_shapes=[
            pltpu.VMEM((rows, depth), BF16),
            pltpu.VMEM((depth, 4 * DK), BF16),
            pltpu.VMEM((2, depth, heads), BF16),
            pltpu.VMEM((RIM, 3 * DK), BF16),
            pltpu.VMEM((RIM, 3 * DK), BF16),
            pltpu.SemaphoreType.DMA((6,)),
            pltpu.SemaphoreType.DMA((parts, 4)),
            pltpu.SemaphoreType.DMA((parts, 4)),
            pltpu.SemaphoreType.DMA((parts, 4)),
            pltpu.SemaphoreType.DMA((parts, 4)),
            pltpu.SemaphoreType.DMA((2,)),
        ],
        compiler_params=pltpu.CompilerParams(collective_id=0, has_side_effects=True),
    )(x, wq, wk, wv, wz, wr)


def inverse_of_unit_lower(a, row, col):
    eye = (row == col).astype(F32)
    size = 8
    y = jnp.where(row // size == col // size, a, 0.0)
    t = eye - y
    y2 = dot3(y, y, BNN)
    t, y4 = t + dot3(t, y2, BNN), dot3(y2, y2, BNN)
    t = t + dot3(t, y4, BNN)
    while size < ROWS:
        joins = (row // (2 * size) == col // (2 * size)) & (row // size != col // size)
        t = t - dot3(t, dot3(jnp.where(joins, a, 0.0), t, BNN), BNN)
        size *= 2
    return t


def scan_kernel(
    raw_ref, rates_ref, rim_ref, taps_ref, speed_ref, logs_ref, gain_ref, probe_ref,
    mixed_ref, cache_ref, read_ref,
    ext, board, own, send_sem, recv_sem,
):
    sp = lax.axis_index("sp")
    tp = lax.axis_index("tp")
    n_sp = lax.axis_size("sp")
    rows = raw_ref.shape[0]
    parts = rows // ROWS
    strides = (1, 4, 16)

    def member(level, turn):
        stride = strides[level]
        digit = (sp // stride) % 4
        return sp + ((digit + turn) % 4 - digit) * stride

    barrier = pltpu.get_barrier_semaphore()
    for level in (2, 1, 0):
        for turn in (2, 1, 3):
            pl.semaphore_signal(
                barrier, inc=1, device_id=(member(level, turn), tp), device_id_type=MESH
            )

    first = (sp == 0).astype(F32)
    ext[pl.ds(0, RIM), :] = rim_ref[...].astype(F32) * (1.0 - first)
    ext[pl.ds(RIM, rows), :] = raw_ref[:, : 3 * DK].astype(F32)
    outs = []
    for c in range(3):
        lanes = pl.ds(c * DK, DK)
        total = jnp.zeros((rows, DK), F32)
        for lag in range(CONV):
            tap = taps_ref[c, pl.ds(lag, 1), :].astype(F32)
            total = total + tap * ext[pl.ds(RIM - (CONV - 1) + lag, rows), lanes]
        outs.append(silu(total))
    query, keys, values = outs
    query = query * (lax.rsqrt(jnp.sum(query * query, axis=-1, keepdims=True) + EPS) * DK**-0.5)
    keys = keys * lax.rsqrt(jnp.sum(keys * keys, axis=-1, keepdims=True) + EPS)

    heads = rates_ref.shape[2]
    mine = lax.broadcasted_iota(jnp.int32, (rows, heads), 1) == tp
    fade = jnp.sum(jnp.where(mine, rates_ref[0], 0.0), axis=-1, keepdims=True)
    write = jnp.sum(jnp.where(mine, rates_ref[1], 0.0), axis=-1, keepdims=True)
    beta = jax.nn.sigmoid(write - math.log(4.0 * rows * n_sp / DK))
    soft = jnp.maximum(fade, 0.0) + jnp.log1p(jnp.exp(-jnp.abs(fade)))
    exponent = logs_ref[...] - speed_ref[tp] * soft

    shape = (parts, ROWS, DK)
    row = lax.broadcasted_iota(jnp.int32, (ROWS, ROWS), 0)
    col = lax.broadcasted_iota(jnp.int32, (ROWS, ROWS), 1)
    eye = (row == col).astype(F32)
    below = (row >= col).astype(BF16)
    spread = jnp.broadcast_to(exponent, (rows, DK)).reshape(shape)
    summed = []
    for part in range(parts):
        high, low = halves(spread[part])
        lowest = (spread[part] - high.astype(F32) - low.astype(F32)).astype(BF16)
        summed.append(dot(below, high, NN) + (dot(below, low, NN) + dot(below, lowest, NN)))
    decay = jnp.stack([jnp.exp(jnp.where(row >= col, s - s.T, -1e30)) for s in summed])
    summed = jnp.stack(summed)
    query, keys, values = (a.reshape(shape) for a in (query, keys, values))
    beta = beta.reshape(parts, ROWS, 1)

    k_beta = keys * beta
    a_mat = jnp.where((row > col)[None], dot3(k_beta, keys, BNT) * decay, 0.0)
    t_mat = inverse_of_unit_lower(a_mat, row[None], col[None])
    grown = jnp.exp(summed)
    right = jnp.concatenate([k_beta * grown, values * beta], axis=2)
    wu = dot3(t_mat, right, BNN)
    k_dec = keys * jnp.exp(summed[:, ROWS - 1 :, :] - summed)
    last = grown[:, ROWS - 1 :, :]

    news, starts, gains = [], [], []
    m = None
    gain = jnp.ones((1, DK), F32)
    for part in range(parts):
        w = wu[part, :, :DK]
        new = jnp.concatenate([gain * w, wu[part, :, DK:]], axis=1)
        if m is not None:
            new = new - dot3(w, m, NN)
        news.append(new)
        starts.append(m)
        gains.append(gain)
        step = dot3(k_dec[part], new, TN)
        twice = jnp.concatenate([last[part], last[part]], axis=1)
        m = step if m is None else twice * m + step
        gain = gain * last[part]

    def post(level, m, gain):
        digit = (sp // strides[level]) % 4
        g2 = jnp.concatenate([gain, gain], axis=1)
        high = g2.astype(BF16).astype(F32)
        mid = (g2 - high).astype(BF16).astype(F32)
        low = g2 - high - mid
        at = lax.broadcasted_iota(jnp.int32, (RIM, 2 * DK), 0)
        extra = jnp.where(at == 0, high, jnp.where(at == 1, mid, jnp.where(at == 2, low, 0.0)))
        board[level, digit, pl.ds(0, DK), :] = m.astype(BF16)
        board[level, digit, pl.ds(DK, RIM), :] = extra.astype(BF16)
        copies = []
        for turn in (2, 1, 3):
            place = board.at[level, digit]
            copy = pltpu.make_async_remote_copy(
                src_ref=place, dst_ref=place,
                send_sem=send_sem.at[level, turn], recv_sem=recv_sem.at[level, turn],
                device_id=(member(level, turn), tp), device_id_type=MESH,
            )
            copy.start()
            copies.append(copy)
        return copies

    def read(level, i):
        transition = board[level, i, pl.ds(0, DK), pl.ds(0, DK)]
        whole = board[level, i, pl.ds(0, DK), :].astype(F32)
        extra = board[level, i, pl.ds(DK, RIM), :].astype(F32)
        return transition, whole, extra[0:1] + extra[1:2] + extra[2:3]

    def apply(transition, g2, m):
        high, low = halves(m)
        return g2 * m - (dot(transition, high, NN) + dot(transition, low, NN))

    def compose(level):
        digit = (sp // strides[level]) % 4
        _, m, gain = read(level, 0)
        before, before_gain = jnp.zeros((DK, 2 * DK), F32), jnp.ones((1, 2 * DK), F32)
        for i in range(1, 4):
            before = jnp.where(digit == i, m, before)
            before_gain = jnp.where(digit == i, gain, before_gain)
            transition, own_m, g2 = read(level, i)
            scaled = jnp.concatenate([gain[:, :DK] * own_m[:, :DK], own_m[:, DK:]], axis=1)
            m = apply(transition, g2, m) + scaled
            gain = gain * g2
        return m, gain[:, :DK], before, before_gain[:, :DK]

    pl.semaphore_wait(barrier, 9)
    copies = post(0, m, gain)

    base, coupling = [], []
    attend = dot3(query, keys, BNT) * decay
    q_dec = query * grown
    for part in range(parts):
        both = dot3(attend[part], news[part], NN)
        if starts[part] is not None:
            both = both + dot3(q_dec[part], starts[part], NN)
        coupling.append(gains[part] * q_dec[part] - both[:, :DK])
        base.append(both[:, DK:])
    coupling = jnp.concatenate(coupling, axis=0)
    base = jnp.concatenate(base, axis=0)
    gate = silu(raw_ref[:, 3 * DK :].astype(F32)) * gain_ref[...].astype(F32)

    sent = list(copies)
    for level in range(2):
        for copy in copies:
            copy.wait_recv()
        m, gain, before, before_gain = compose(level)
        copies = post(level + 1, m, gain)
        sent += copies
        both = dot3(coupling, before, NN)
        coupling = before_gain * coupling - both[:, :DK]
        base = base + both[:, DK:]
    for copy in copies:
        copy.wait_recv()

    digit = (sp // strides[2]) % 4
    state = board[2, 0, pl.ds(0, DK), pl.ds(DK, DK)].astype(F32)
    entry = jnp.zeros((DK, DK), F32)
    for i in range(1, 4):
        entry = jnp.where(digit == i, state, entry)
        transition, whole, g2 = read(2, i)
        state = apply(transition, g2[:, :DK], state) + whole[:, DK:]
    out = base + dot3(coupling, entry, NN)
    normed = out * lax.rsqrt(jnp.mean(out * out, axis=-1, keepdims=True) + EPS)
    mixed_ref[...] = (normed * gate).astype(BF16)
    cache = state.astype(BF16)
    cache_ref[0] = cache
    probe = probe_ref[0].astype(F32)
    probe = probe * (lax.rsqrt(jnp.sum(probe * probe, axis=-1, keepdims=True) + EPS) * DK**-0.5)
    high, low = halves(jnp.broadcast_to(probe, (16, DK)))
    read_ref[0] = (dot(high, cache, NN) + dot(low, cache, NN))[0:1]
    for copy in sent:
        copy.wait_send()


def scan(raw, rates, rim, taps, speed, logs, gain, probe):
    rows = raw.shape[0]
    vmem = pl.BlockSpec(memory_space=pltpu.VMEM)
    smem = pl.BlockSpec(memory_space=pltpu.SMEM)
    return pl.pallas_call(
        scan_kernel,
        out_shape=(
            jax.ShapeDtypeStruct((rows, DK), BF16),
            jax.ShapeDtypeStruct((1, DK, DK), BF16),
            jax.ShapeDtypeStruct((1, 1, DK), F32),
        ),
        in_specs=[vmem, vmem, vmem, vmem, smem, vmem, vmem, vmem],
        out_specs=(vmem, vmem, vmem),
        scratch_shapes=[
            pltpu.VMEM((rows + RIM, 3 * DK), F32),
            pltpu.VMEM((3, 4, DK + RIM, 2 * DK), BF16),
            pltpu.VMEM((8, DK), F32),
            pltpu.SemaphoreType.DMA((3, 4)),
            pltpu.SemaphoreType.DMA((3, 4)),
        ],
        compiler_params=pltpu.CompilerParams(collective_id=1, has_side_effects=True),
    )(raw, rates, rim, taps, speed, logs, gain, probe)


def on_device(x, wq, wk, wv, wz, wr, taps, speed, logs, gain, probe):
    raw, rates, rim = project(x, wq, wk, wv, wz, wr)
    return scan(raw, rates, rim, taps, speed, logs, gain.reshape(1, DK), probe)


def solution(mesh):
    in_specs = (
        P("sp", "tp"),
        P(None, "tp"),
        P(None, "tp"),
        P(None, "tp"),
        P(None, "tp"),
        P(),
        P(None, None, "tp"),
        P(),
        P("sp", "tp"),
        P(),
        P("sp", "tp", None),
    )
    out_specs = (P("sp", "tp"), P("tp", None, None), P("sp", "tp", None))
    return jax.shard_map(
        on_device, mesh=mesh, in_specs=in_specs, out_specs=out_specs, check_vma=False
    )
```

```python
import functools
import math

import jax
import jax.numpy as jnp
from jax import lax
from jax.experimental import pallas as pl
from jax.experimental.pallas import tpu as pltpu
from jax.sharding import PartitionSpec as P

DK = 128
CONV = 4
EPS = 1e-06
MESH = pl.DeviceIdType.MESH
F32 = jnp.float32
BF16 = jnp.bfloat16

ROWS = 128
RIM = 16
EXTRA = 8
TOKENS = True
SHARE = DK // 4


def silu(value):
    return value * jax.nn.sigmoid(value)


def halves(value):
    high = value.astype(BF16)
    low = (value - high.astype(F32)).astype(BF16)
    return high, low


def dot(left, right, dims):
    return lax.dot_general(left, right, dims, preferred_element_type=F32)


def dot3(left, right, dims):
    lh, ll = halves(left)
    rh, rl = halves(right)
    return dot(lh, rh, dims) + (dot(lh, rl, dims) + dot(ll, rh, dims))


def dot2(left, right, dims):
    lh, ll = halves(left)
    right = right.astype(BF16)
    left = jnp.concatenate([lh, ll], axis=-1)
    return dot(left, jnp.concatenate([right, right], axis=-2), dims)


NN = (((1,), (0,)), ((), ()))
NT = (((1,), (1,)), ((), ()))
TN = (((0,), (0,)), ((), ()))
BNN = (((2,), (1,)), ((0,), (0,)))
BNT = (((2,), (2,)), ((0,), (0,)))


def inverse_of_unit_lower(a, row, col):
    eye = (row == col).astype(F32)
    size = 8
    y = jnp.where(row // size == col // size, a, 0.0)
    t = eye - y
    y2 = dot3(y, y, BNN)
    t, y4 = t + dot3(t, y2, BNN), dot3(y2, y2, BNN)
    t = t + dot3(t, y4, BNN)
    while size < ROWS:
        joins = (row // (2 * size) == col // (2 * size)) & (row // size != col // size)
        t = t - dot2(t, dot2(jnp.where(joins, a, 0.0), t, BNN), BNN)
        size *= 2
    return t


def kernel(
    x_hbm, wq_hbm, wk_hbm, wv_hbm, wz_hbm, wr_hbm,
    taps_ref, speed_ref, logs_ref, gain_ref, probe_ref,
    mixed_ref, cache_ref, read_ref,
    x_all, x_tail, w_all, w_rate, tail, rim_in, ext, gates,
    q_ref, k_ref, kb_ref, vb_ref, a_ref, sum_ref, decay_ref,
    board_0, board_1, board_2,
    load_sem, near_send, near_recv, core_send, core_recv, rim_sem,
    send_sem, recv_sem, pass_sem, got_sem, token,
):
    sp = lax.axis_index("sp")
    tp = lax.axis_index("tp")
    n_sp = lax.axis_size("sp")
    chip, core = tp // 2, tp % 2
    partner = chip * 2 + (1 - core)
    rows, width = x_hbm.shape
    parts = rows // ROWS
    strides, counts = (1, 4, 8), (4, 2, n_sp // 8)
    far = counts[2]
    digits = [(sp // stride) % count for stride, count in zip(strides, counts)]
    turns = [
        (2, 1, 3),
        (1,),
        sorted(range(1, far), key=lambda turn: min(turn, far - turn)),
    ]

    def member(level, turn):
        digit = digits[level]
        return sp + ((digit + turn) % counts[level] - digit) * strides[level]

    def columns(slot):
        return pl.ds(pl.multiple_of(slot * width, width), width)

    def near(r):
        return ((chip + r) % 4) * 2 + core

    load_x = pltpu.make_async_copy(x_hbm, x_all.at[:, columns(tp)], load_sem.at[0])
    load_x.start()
    load_tail = pltpu.make_async_copy(
        x_hbm.at[pl.ds(rows - RIM, RIM), :], x_tail.at[:, columns(tp)], load_sem.at[6]
    )
    load_tail.start()
    loads = []
    for i, w in enumerate((wq_hbm, wk_hbm, wv_hbm, wz_hbm)):
        loads.append(
            pltpu.make_async_copy(w, w_all.at[:, pl.ds(i * DK, DK)], load_sem.at[1 + i])
        )
    loads.append(pltpu.make_async_copy(wr_hbm, w_rate, load_sem.at[5]))
    for load in loads:
        load.start()

    after, before_sp = (sp + 1) % n_sp, (sp + n_sp - 1) % n_sp
    barrier = pltpu.get_barrier_semaphore()
    greeted = [(sp, near(r)) for r in (2, 1, 3)] + [(sp, partner), (after, tp), (before_sp, tp)]
    greeted += [(member(0, turn), tp) for turn in turns[0]] + [(member(1, 1), tp)]
    beyond = (1, far - 1) if TOKENS else turns[2]
    greeted += [(member(2, turn), tp) for turn in beyond]
    for peer in greeted:
        pl.semaphore_signal(barrier, inc=1, device_id=peer, device_id_type=MESH)
    load_x.wait()
    load_tail.wait()
    pl.semaphore_wait(barrier, len(greeted))

    def pass_token(i):
        if TOKENS and 0 < i < far // 2:
            pl.semaphore_wait(token.at[i - 1], 2)
        if TOKENS and i < far // 2 - 1:
            for turn in (1, far - 1):
                pl.semaphore_signal(
                    token.at[i], inc=1, device_id=(member(2, turn), tp), device_id_type=MESH
                )

    def block(part, slot):
        if part == parts:
            return x_tail.at[:, columns(slot)]
        return x_all.at[pl.ds(part * ROWS, ROWS), columns(slot)]

    def to(place, peer, send, recv):
        copy = pltpu.make_async_remote_copy(
            src_ref=place, dst_ref=place, send_sem=send, recv_sem=recv,
            device_id=(sp, peer), device_id_type=MESH,
        )
        copy.start()
        return copy

    sends, passes = {}, []
    order = [parts] + list(range(parts))
    for part in order:
        for r in (2, 1, 3):
            sends[part, r] = to(
                block(part, tp), near(r), near_send.at[part, r], near_recv.at[part, r]
            )
        sends[part, 0] = to(
            block(part, tp), partner, core_send.at[part, 0], core_recv.at[part, 0]
        )
    pass_token(0)
    for load in loads:
        load.wait()

    def gathered(part):
        mine = []
        for r in (1, 3, 2):
            sends[part, r].wait_recv()
            slot = ((chip + 4 - r) % 4) * 2 + core
            mine.append(
                to(block(part, slot), partner, core_send.at[part, r], core_recv.at[part, r])
            )
        sends[part, 0].wait_recv()
        for copy in mine:
            copy.wait_recv()
        passes.extend(mine)

    gathered(parts)
    tail[...] = dot(x_tail[...], w_all[:, pl.ds(0, 3 * DK)], NN).astype(BF16)
    rim_copy = pltpu.make_async_remote_copy(
        src_ref=tail, dst_ref=rim_in, send_sem=rim_sem.at[0], recv_sem=rim_sem.at[1],
        device_id=(after, tp), device_id_type=MESH,
    )
    rim_copy.start()
    pass_token(1)

    row = lax.broadcasted_iota(jnp.int32, (ROWS, ROWS), 0)
    col = lax.broadcasted_iota(jnp.int32, (ROWS, ROWS), 1)
    eye = (row == col).astype(F32)
    below = (row >= col).astype(BF16)
    gain_row = gain_ref[...].astype(F32)

    def prepare(part):
        here = pl.ds(part * ROWS, ROWS)
        x = x_all[here, :]
        raw = dot(x, w_all[...], NN).astype(BF16).astype(F32)
        rates = dot(x, w_rate[...], NT)
        ext[pl.ds(RIM + part * ROWS, ROWS), :] = raw[:, : 3 * DK]
        gates[here, :] = silu(raw[:, 3 * DK :]) * gain_row
        outs = []
        for c in range(3):
            lanes = pl.ds(c * DK, DK)
            total = jnp.zeros((ROWS, DK), F32)
            for lag in range(CONV):
                tap = taps_ref[c, pl.ds(lag, 1), :].astype(F32)
                total = total + tap * ext[
                    pl.ds(part * ROWS + RIM - (CONV - 1) + lag, ROWS), lanes
                ]
            outs.append(silu(total))
        query, keys, values = outs
        query = query * (
            lax.rsqrt(jnp.sum(query * query, axis=-1, keepdims=True) + EPS) * DK**-0.5
        )
        keys = keys * lax.rsqrt(jnp.sum(keys * keys, axis=-1, keepdims=True) + EPS)
        kinds = rates.shape[1]
        kind = lax.broadcasted_iota(jnp.int32, (ROWS, kinds), 1)
        fade = jnp.sum(jnp.where(kind == tp, rates, 0.0), axis=-1, keepdims=True)
        write = jnp.sum(jnp.where(kind == tp + kinds // 2, rates, 0.0), axis=-1, keepdims=True)
        beta = jax.nn.sigmoid(write - math.log(4.0 * rows * n_sp / DK))
        soft = jnp.maximum(fade, 0.0) + jnp.log1p(jnp.exp(-jnp.abs(fade)))
        spread = jnp.broadcast_to(logs_ref[:, here], (ROWS, ROWS)).T - speed_ref[tp] * soft
        high, low = halves(spread)
        lowest = (spread - high.astype(F32) - low.astype(F32)).astype(BF16)
        summed = dot(below, high, NN) + (dot(below, low, NN) + dot(below, lowest, NN))
        decay = jnp.exp(jnp.where(row >= col, summed - summed.T, -1e30))
        k_beta = keys * beta
        q_ref[part] = query
        k_ref[part] = keys
        kb_ref[part] = k_beta
        vb_ref[part] = values * beta
        sum_ref[part] = summed
        decay_ref[part] = decay
        a_ref[part] = jnp.where(row > col, dot3(k_beta, keys, NT) * decay, 0.0)

    for part in range(parts):
        gathered(part)
        if part == 0:
            rim_copy.wait_recv()
            ext[pl.ds(0, RIM), :] = jnp.where(sp == 0, 0.0, rim_in[...].astype(F32))
        prepare(part)
        pass_token(part + 2)

    query, keys, k_beta, summed, decay = (
        ref[...] for ref in (q_ref, k_ref, kb_ref, sum_ref, decay_ref)
    )
    t_mat = inverse_of_unit_lower(a_ref[...], row[None], col[None])
    grown = jnp.exp(summed)
    right = jnp.concatenate([k_beta * grown, vb_ref[...]], axis=2)
    wu = dot3(t_mat, right, BNN)
    k_dec = keys * jnp.exp(summed[:, ROWS - 1 :, :] - summed)
    last = grown[:, ROWS - 1 :, :]

    news, starts, gains = [], [], []
    m = None
    gain = jnp.ones((1, DK), F32)
    for part in range(parts):
        w = wu[part, :, :DK]
        new = jnp.concatenate([gain * w, wu[part, :, DK:]], axis=1)
        if m is not None:
            new = new - dot3(w, m, NN)
        news.append(new)
        starts.append(m)
        gains.append(gain)
        step = dot3(k_dec[part], new, TN)
        twice = jnp.concatenate([last[part], last[part]], axis=1)
        m = step if m is None else twice * m + step
        gain = gain * last[part]

    def gain_rows(gain):
        g2 = jnp.concatenate([gain, gain], axis=1)
        high = g2.astype(BF16).astype(F32)
        mid = (g2 - high).astype(BF16).astype(F32)
        low = g2 - high - mid
        at = lax.broadcasted_iota(jnp.int32, (EXTRA, 2 * DK), 0)
        extra = jnp.where(at == 0, high, jnp.where(at == 1, mid, jnp.where(at == 2, low, 0.0)))
        return extra.astype(BF16)

    def gain_of(extra):
        extra = extra.astype(F32)
        return extra[0:1] + extra[1:2] + extra[2:3]

    boards = (board_0, board_1)

    def remote(place, level, turn, send, recv):
        copy = pltpu.make_async_remote_copy(
            src_ref=place, dst_ref=place, send_sem=send, recv_sem=recv,
            device_id=(member(level, turn), tp), device_id_type=MESH,
        )
        copy.start()
        return copy

    def post(level, m, gain):
        board, digit = boards[level], digits[level]
        board[digit, pl.ds(0, DK), :] = m.astype(BF16)
        board[digit, pl.ds(DK, EXTRA), :] = gain_rows(gain)
        return [
            remote(
                board.at[digit], level, turn,
                send_sem.at[level, turn], recv_sem.at[level, turn],
            )
            for turn in turns[level]
        ]

    def post_quarters(m, gain):
        rounded, extra = m.astype(BF16), gain_rows(gain)
        for i in range(4):
            board_2[digits[2], i, pl.ds(0, SHARE), :] = rounded[i * SHARE : (i + 1) * SHARE]
            board_2[digits[2], i, pl.ds(SHARE, EXTRA), :] = extra
        place = board_2.at[digits[2], digits[0]]
        return {
            turn: remote(place, 2, turn, send_sem.at[2, turn], recv_sem.at[2, turn])
            for turn in turns[2]
        }

    def read(level, i):
        board = boards[level]
        transition = board[i, pl.ds(0, DK), pl.ds(0, DK)]
        whole = board[i, pl.ds(0, DK), :].astype(F32)
        return transition, whole, gain_of(board[i, pl.ds(DK, EXTRA), :])

    def apply(transition, g2, m):
        high, low = halves(m)
        wide = jnp.concatenate([transition, transition], axis=1)
        return g2 * m - dot(wide, jnp.concatenate([high, low], axis=0), NN)

    def compose(level):
        digit = digits[level]
        _, m, gain = read(level, 0)
        before, before_gain = jnp.zeros((DK, 2 * DK), F32), jnp.ones((1, 2 * DK), F32)
        for i in range(1, counts[level]):
            before = jnp.where(digit == i, m, before)
            before_gain = jnp.where(digit == i, gain, before_gain)
            transition, own_m, g2 = read(level, i)
            scaled = jnp.concatenate([gain[:, :DK] * own_m[:, :DK], own_m[:, DK:]], axis=1)
            m = apply(transition, g2, m) + scaled
            gain = gain * g2
        return m, gain[:, :DK], before, before_gain[:, :DK]

    copies = post(0, m, gain)

    base, coupling = [], []
    attend = dot3(query, keys, BNT) * decay
    q_dec = query * grown
    for part in range(parts):
        both = dot3(attend[part], news[part], NN)
        if starts[part] is not None:
            both = both + dot3(q_dec[part], starts[part], NN)
        coupling.append(gains[part] * q_dec[part] - both[:, :DK])
        base.append(both[:, DK:])
    coupling = jnp.concatenate(coupling, axis=0)
    base = jnp.concatenate(base, axis=0)

    sent = list(copies)
    for level in range(2):
        for copy in copies:
            copy.wait_recv()
        m, gain, before, before_gain = compose(level)
        if level == 0:
            copies = post(1, m, gain)
            sent += copies
        else:
            quarters = post_quarters(m, gain)
            sent += list(quarters.values())
        both = dot3(coupling, before, NN)
        coupling = before_gain * coupling - both[:, :DK]
        base = base + both[:, DK:]
    passed = []
    for turn in turns[2]:
        quarters[turn].wait_recv()
        place = board_2.at[(digits[2] + far - turn) % far, digits[0]]
        for side in turns[0]:
            passed.append(
                remote(place, 0, side, pass_sem.at[turn, side], got_sem.at[turn, side])
            )
    for copy in passed:
        copy.wait_recv()
    sent += passed

    def part_of(i, lanes):
        return board_2[i, :, pl.ds(0, SHARE), lanes].reshape(DK, DK)

    state = part_of(0, pl.ds(DK, DK)).astype(F32)
    entry = jnp.zeros((DK, DK), F32)
    for i in range(1, far):
        entry = jnp.where(digits[2] == i, state, entry)
        g2 = gain_of(board_2[i, 0, pl.ds(SHARE, EXTRA), pl.ds(0, DK)])
        added = part_of(i, pl.ds(DK, DK)).astype(F32)
        state = apply(part_of(i, pl.ds(0, DK)), g2, state) + added
    out = base + dot3(coupling, entry, NN)
    normed = out * lax.rsqrt(jnp.mean(out * out, axis=-1, keepdims=True) + EPS)
    mixed_ref[...] = (normed * gates[...]).astype(BF16)
    cache = state.astype(BF16)
    cache_ref[0] = cache
    probe = probe_ref[0].astype(F32)
    probe = probe * (lax.rsqrt(jnp.sum(probe * probe, axis=-1, keepdims=True) + EPS) * DK**-0.5)
    high, low = halves(jnp.broadcast_to(probe, (16, DK)))
    read_ref[0] = (dot(high, cache, NN) + dot(low, cache, NN))[0:1]
    rim_copy.wait_send()
    for copy in sent + passes + list(sends.values()):
        copy.wait_send()


def fused(x, wq, wk, wv, wz, wr, taps, speed, logs, gain, probe):
    rows = x.shape[0]
    depth = wq.shape[0]
    parts = rows // ROWS
    any_space = pl.BlockSpec(memory_space=pl.ANY)
    vmem = pl.BlockSpec(memory_space=pltpu.VMEM)
    smem = pl.BlockSpec(memory_space=pltpu.SMEM)
    dma = pltpu.SemaphoreType.DMA
    block = pltpu.VMEM((parts, ROWS, DK), F32)
    return pl.pallas_call(
        kernel,
        out_shape=(
            jax.ShapeDtypeStruct((rows, DK), BF16),
            jax.ShapeDtypeStruct((1, DK, DK), BF16),
            jax.ShapeDtypeStruct((1, 1, DK), F32),
        ),
        in_specs=[any_space] * 6 + [vmem, smem, vmem, vmem, vmem],
        out_specs=(vmem, vmem, vmem),
        scratch_shapes=[
            pltpu.VMEM((rows, depth), BF16),
            pltpu.VMEM((RIM, depth), BF16),
            pltpu.VMEM((depth, 4 * DK), BF16),
            pltpu.VMEM(wr.shape, BF16),
            pltpu.VMEM((RIM, 3 * DK), BF16),
            pltpu.VMEM((RIM, 3 * DK), BF16),
            pltpu.VMEM((rows + RIM, 3 * DK), F32),
            pltpu.VMEM((rows, DK), F32),
            *[block] * 7,
            pltpu.VMEM((4, DK + EXTRA, 2 * DK), BF16),
            pltpu.VMEM((2, DK + EXTRA, 2 * DK), BF16),
            pltpu.VMEM((8, 4, SHARE + EXTRA, 2 * DK), BF16),
            dma((7,)),
            dma((parts + 1, 4)),
            dma((parts + 1, 4)),
            dma((parts + 1, 4)),
            dma((parts + 1, 4)),
            dma((2,)),
            dma((3, 8)),
            dma((3, 8)),
            dma((8, 4)),
            dma((8, 4)),
            pltpu.SemaphoreType.REGULAR((4,)),
        ],
        compiler_params=pltpu.CompilerParams(collective_id=0, has_side_effects=True),
    )(x, wq, wk, wv, wz, wr, taps, speed, logs, gain, probe)


def on_device(x, wq, wk, wv, wz, wr, taps, speed, logs, gain, probe):
    by_kind = wr.transpose(0, 2, 1).reshape(-1, wr.shape[1])
    return fused(
        x, wq, wk, wv, wz, by_kind, taps, speed, logs.reshape(1, -1), gain.reshape(1, DK), probe
    )


def solution(mesh):
    in_specs = (
        P("sp", "tp"),
        P(None, "tp"),
        P(None, "tp"),
        P(None, "tp"),
        P(None, "tp"),
        P(),
        P(None, None, "tp"),
        P(),
        P("sp", "tp"),
        P(),
        P("sp", "tp", None),
    )
    out_specs = (P("sp", "tp"), P("tp", None, None), P("sp", "tp", None))
    return jax.shard_map(
        on_device, mesh=mesh, in_specs=in_specs, out_specs=out_specs, check_vma=False
    )
```

```python
import functools
import math

import jax
import jax.numpy as jnp
from jax import lax
from jax.experimental import pallas as pl
from jax.experimental.pallas import tpu as pltpu
from jax.sharding import PartitionSpec as P

DK = 128
CONV = 4
EPS = 1e-06
MESH = pl.DeviceIdType.MESH
F32 = jnp.float32
BF16 = jnp.bfloat16

ROWS = 128
RIM = 16
EXTRA = 8
TOKENS = True
SHARE = DK // 4


def silu(value):
    return value * jax.nn.sigmoid(value)


def halves(value):
    high = value.astype(BF16)
    low = (value - high.astype(F32)).astype(BF16)
    return high, low


def dot(left, right, dims):
    return lax.dot_general(left, right, dims, preferred_element_type=F32)


def dot3(left, right, dims):
    lh, ll = halves(left)
    rh, rl = halves(right)
    return dot(lh, rh, dims) + (dot(lh, rl, dims) + dot(ll, rh, dims))


def dot2(left, right, dims):
    lh, ll = halves(left)
    right = right.astype(BF16)
    left = jnp.concatenate([lh, ll], axis=-1)
    return dot(left, jnp.concatenate([right, right], axis=-2), dims)


NN = (((1,), (0,)), ((), ()))
NT = (((1,), (1,)), ((), ()))
TN = (((0,), (0,)), ((), ()))
BNN = (((2,), (1,)), ((0,), (0,)))
BNT = (((2,), (2,)), ((0,), (0,)))


def inverse_of_unit_lower(a, row, col):
    eye = (row == col).astype(F32)
    size = 8
    y = jnp.where(row // size == col // size, a, 0.0)
    t = eye - y
    y2 = dot3(y, y, BNN)
    t, y4 = t + dot3(t, y2, BNN), dot3(y2, y2, BNN)
    t = t + dot3(t, y4, BNN)
    while size < ROWS:
        joins = (row // (4 * size) == col // (4 * size)) & (row // size != col // size)
        n = dot2(t, jnp.where(joins, a, 0.0), BNN)
        t, n2 = t - dot2(n, t, BNN), dot2(n, n, BNN)
        t = t + dot2(n2, t, BNN)
        size *= 4
    return t


def kernel(
    x_hbm, wq_hbm, wk_hbm, wv_hbm, wz_hbm, wr_hbm,
    taps_hbm, speed_hbm, logs_hbm, gain_hbm, probe_hbm,
    mixed_ref, cache_ref, read_ref,
    taps_ref, speed_ref, logs_ref, gain_ref, probe_ref,
    x_all, x_tail, w_all, w_rate, tail, rim_in, ext, gates,
    q_ref, k_ref, kb_ref, vb_ref, a_ref, sum_ref, decay_ref,
    board_0, board_1, board_2,
    load_sem, near_send, near_recv, core_send, core_recv, rim_sem,
    send_sem, recv_sem, pass_sem, got_sem, token,
):
    sp = lax.axis_index("sp")
    tp = lax.axis_index("tp")
    n_sp = lax.axis_size("sp")
    chip, core = tp // 2, tp % 2
    partner = chip * 2 + (1 - core)
    rows, width = x_hbm.shape
    parts = rows // ROWS
    strides, counts = (1, 4, 8), (4, 2, n_sp // 8)
    far = counts[2]
    digits = [(sp // stride) % count for stride, count in zip(strides, counts)]
    turns = [
        (2, 1, 3),
        (1,),
        sorted(range(1, far), key=lambda turn: min(turn, far - turn)),
    ]

    def member(level, turn):
        digit = digits[level]
        return sp + ((digit + turn) % counts[level] - digit) * strides[level]

    def near(r):
        return ((chip + r) % 4) * 2 + core

    load_x = pltpu.make_async_copy(x_hbm, x_all.at[tp], load_sem.at[0])
    load_x.start()
    load_tail = pltpu.make_async_copy(
        x_hbm.at[pl.ds(rows - RIM, RIM), :], x_tail.at[tp], load_sem.at[6]
    )
    load_tail.start()
    after, before_sp = (sp + 1) % n_sp, (sp + n_sp - 1) % n_sp
    barrier = pltpu.get_barrier_semaphore()
    greeted = [(sp, near(r)) for r in (2, 1, 3)] + [(sp, partner), (after, tp), (before_sp, tp)]
    greeted += [(member(0, turn), tp) for turn in turns[0]] + [(member(1, 1), tp)]
    beyond = (1, far - 1) if TOKENS else turns[2]
    greeted += [(member(2, turn), tp) for turn in beyond]
    for peer in greeted:
        pl.semaphore_signal(barrier, inc=1, device_id=peer, device_id_type=MESH)
    loads = []
    for i, w in enumerate((wq_hbm, wk_hbm, wv_hbm, wz_hbm)):
        loads.append(
            pltpu.make_async_copy(w, w_all.at[i], load_sem.at[1 + i])
        )
    loads.append(pltpu.make_async_copy(wr_hbm, w_rate, load_sem.at[5]))
    small = (
        (taps_hbm, taps_ref), (speed_hbm, speed_ref), (logs_hbm, logs_ref),
        (gain_hbm, gain_ref), (probe_hbm, probe_ref),
    )
    for i, (source, place) in enumerate(small):
        loads.append(pltpu.make_async_copy(source, place, load_sem.at[7 + i]))
    for load in loads:
        load.start()

    load_x.wait()
    load_tail.wait()
    pl.semaphore_wait(barrier, len(greeted))

    def pass_token(i):
        if TOKENS and 0 < i < far // 2:
            pl.semaphore_wait(token.at[i - 1], 2)
        if TOKENS and i < far // 2 - 1:
            for turn in (1, far - 1):
                pl.semaphore_signal(
                    token.at[i], inc=1, device_id=(member(2, turn), tp), device_id_type=MESH
                )

    def block(part, slot):
        if part == parts:
            return x_tail.at[slot]
        return x_all.at[slot, pl.ds(part * ROWS, ROWS)]

    def to(place, peer, send, recv):
        copy = pltpu.make_async_remote_copy(
            src_ref=place, dst_ref=place, send_sem=send, recv_sem=recv,
            device_id=(sp, peer), device_id_type=MESH,
        )
        copy.start()
        return copy

    sends, passes = {}, []
    order = [parts] + list(range(parts))
    for part in order:
        for r in (2, 1, 3):
            sends[part, r] = to(
                block(part, tp), near(r), near_send.at[part, r], near_recv.at[part, r]
            )
        sends[part, 0] = to(
            block(part, tp), partner, core_send.at[part, 0], core_recv.at[part, 0]
        )
    pass_token(0)
    for load in loads:
        load.wait()

    def gathered(part):
        mine = []
        for r in (1, 3, 2):
            sends[part, r].wait_recv()
            slot = ((chip + 4 - r) % 4) * 2 + core
            mine.append(
                to(block(part, slot), partner, core_send.at[part, r], core_recv.at[part, r])
            )
        sends[part, 0].wait_recv()
        for copy in mine:
            copy.wait_recv()
        passes.extend(mine)

    gathered(parts)
    slots = x_all.shape[0]
    tail_x = jnp.concatenate([x_tail[slot] for slot in range(slots)], axis=1)
    three = jnp.concatenate([w_all[i] for i in range(3)], axis=1)
    tail[...] = dot(tail_x, three, NN).astype(BF16)
    rim_copy = pltpu.make_async_remote_copy(
        src_ref=tail, dst_ref=rim_in, send_sem=rim_sem.at[0], recv_sem=rim_sem.at[1],
        device_id=(after, tp), device_id_type=MESH,
    )
    rim_copy.start()
    pass_token(1)

    row = lax.broadcasted_iota(jnp.int32, (ROWS, ROWS), 0)
    col = lax.broadcasted_iota(jnp.int32, (ROWS, ROWS), 1)
    eye = (row == col).astype(F32)
    below = (row >= col).astype(BF16)
    gain_row = gain_ref[...].astype(F32)
    own_head = lax.broadcasted_iota(jnp.int32, speed_ref.shape, 1) == tp
    speed = jnp.sum(jnp.where(own_head, speed_ref[...], 0.0), axis=-1, keepdims=True)

    def prepare(part):
        here = pl.ds(part * ROWS, ROWS)
        x = jnp.concatenate([x_all[slot, here, :] for slot in range(slots)], axis=1)
        four = jnp.concatenate([w_all[i] for i in range(4)], axis=1)
        raw = dot(x, four, NN).astype(BF16).astype(F32)
        rates = dot(x, w_rate[...], NT)
        ext[pl.ds(RIM + part * ROWS, ROWS), :] = raw[:, : 3 * DK]
        gates[here, :] = silu(raw[:, 3 * DK :]) * gain_row
        outs = []
        for c in range(3):
            lanes = pl.ds(c * DK, DK)
            total = jnp.zeros((ROWS, DK), F32)
            for lag in range(CONV):
                tap = taps_ref[c, pl.ds(lag, 1), :].astype(F32)
                total = total + tap * ext[
                    pl.ds(part * ROWS + RIM - (CONV - 1) + lag, ROWS), lanes
                ]
            outs.append(silu(total))
        query, keys, values = outs
        query = query * (
            lax.rsqrt(jnp.sum(query * query, axis=-1, keepdims=True) + EPS) * DK**-0.5
        )
        keys = keys * lax.rsqrt(jnp.sum(keys * keys, axis=-1, keepdims=True) + EPS)
        kinds = rates.shape[1]
        kind = lax.broadcasted_iota(jnp.int32, (ROWS, kinds), 1)
        fade = jnp.sum(jnp.where(kind == tp, rates, 0.0), axis=-1, keepdims=True)
        write = jnp.sum(jnp.where(kind == tp + kinds // 2, rates, 0.0), axis=-1, keepdims=True)
        beta = jax.nn.sigmoid(write - math.log(4.0 * rows * n_sp / DK))
        soft = jnp.maximum(fade, 0.0) + jnp.log1p(jnp.exp(-jnp.abs(fade)))
        spread = jnp.broadcast_to(logs_ref[:, here], (ROWS, ROWS)).T - speed * soft
        high, low = halves(spread)
        lowest = (spread - high.astype(F32) - low.astype(F32)).astype(BF16)
        summed = dot(below, high, NN) + (dot(below, low, NN) + dot(below, lowest, NN))
        decay = jnp.exp(jnp.where(row >= col, summed - summed.T, -1e30))
        k_beta = keys * beta
        q_ref[part] = query
        k_ref[part] = keys
        kb_ref[part] = k_beta
        vb_ref[part] = values * beta
        sum_ref[part] = summed
        decay_ref[part] = decay
        a_ref[part] = jnp.where(row > col, dot3(k_beta, keys, NT) * decay, 0.0)

    for part in range(parts):
        gathered(part)
        if part == 0:
            rim_copy.wait_recv()
            ext[pl.ds(0, RIM), :] = jnp.where(sp == 0, 0.0, rim_in[...].astype(F32))
        prepare(part)
        pass_token(part + 2)

    query, keys, k_beta, summed, decay = (
        ref[...] for ref in (q_ref, k_ref, kb_ref, sum_ref, decay_ref)
    )
    t_mat = inverse_of_unit_lower(a_ref[...], row[None], col[None])
    grown = jnp.exp(summed)
    right = jnp.concatenate([k_beta * grown, vb_ref[...]], axis=2)
    wu = dot2(t_mat, right, BNN)
    k_dec = keys * jnp.exp(summed[:, ROWS - 1 :, :] - summed)
    last = grown[:, ROWS - 1 :, :]

    starts, gains = [], []
    m, gain = None, jnp.ones((1, DK), F32)
    for part in range(parts):
        step = dot3(k_dec[part], wu[part], TN)
        starts.append(m)
        gains.append(gain)
        if m is None:
            m = step
        else:
            twice = jnp.concatenate([last[part], last[part]], axis=1)
            scaled = jnp.concatenate([gain * step[:, :DK], step[:, DK:]], axis=1)
            m = twice * m - dot2(step[:, :DK], m, NN) + scaled
        gain = gain * last[part]

    def gain_rows(gain):
        g2 = jnp.concatenate([gain, gain], axis=1)
        high = g2.astype(BF16).astype(F32)
        mid = (g2 - high).astype(BF16).astype(F32)
        low = g2 - high - mid
        at = lax.broadcasted_iota(jnp.int32, (EXTRA, 2 * DK), 0)
        extra = jnp.where(at == 0, high, jnp.where(at == 1, mid, jnp.where(at == 2, low, 0.0)))
        return extra.astype(BF16)

    def gain_of(extra):
        extra = extra.astype(F32)
        return extra[0:1] + extra[1:2] + extra[2:3]

    boards = (board_0, board_1)

    def remote(place, level, turn, send, recv):
        copy = pltpu.make_async_remote_copy(
            src_ref=place, dst_ref=place, send_sem=send, recv_sem=recv,
            device_id=(member(level, turn), tp), device_id_type=MESH,
        )
        copy.start()
        return copy

    def post(level, m, gain):
        board, digit = boards[level], digits[level]
        board[digit, pl.ds(0, DK), :] = m.astype(BF16)
        board[digit, pl.ds(DK, EXTRA), :] = gain_rows(gain)
        return [
            remote(
                board.at[digit], level, turn,
                send_sem.at[level, turn], recv_sem.at[level, turn],
            )
            for turn in turns[level]
        ]

    def post_quarters(m, gain):
        rounded, extra = m.astype(BF16), gain_rows(gain)
        for i in range(4):
            board_2[digits[2], i, pl.ds(0, SHARE), :] = rounded[i * SHARE : (i + 1) * SHARE]
            board_2[digits[2], i, pl.ds(SHARE, EXTRA), :] = extra
        place = board_2.at[digits[2], digits[0]]
        return {
            turn: remote(place, 2, turn, send_sem.at[2, turn], recv_sem.at[2, turn])
            for turn in turns[2]
        }

    def read(level, i):
        board = boards[level]
        transition = board[i, pl.ds(0, DK), pl.ds(0, DK)]
        whole = board[i, pl.ds(0, DK), :].astype(F32)
        return transition, whole, gain_of(board[i, pl.ds(DK, EXTRA), :])

    def apply(transition, g2, m):
        high, low = halves(m)
        wide = jnp.concatenate([transition, transition], axis=1)
        return g2 * m - dot(wide, jnp.concatenate([high, low], axis=0), NN)

    def compose(level):
        digit = digits[level]
        _, m, gain = read(level, 0)
        before, before_gain = jnp.zeros((DK, 2 * DK), F32), jnp.ones((1, 2 * DK), F32)
        for i in range(1, counts[level]):
            before = jnp.where(digit == i, m, before)
            before_gain = jnp.where(digit == i, gain, before_gain)
            transition, own_m, g2 = read(level, i)
            scaled = jnp.concatenate([gain[:, :DK] * own_m[:, :DK], own_m[:, DK:]], axis=1)
            m = apply(transition, g2, m) + scaled
            gain = gain * g2
        return m, gain[:, :DK], before, before_gain[:, :DK]

    copies = post(0, m, gain)

    base, coupling = [], []
    attend = dot3(query, keys, BNT) * decay
    q_dec = query * grown
    for part in range(parts):
        w = wu[part, :, :DK]
        new = jnp.concatenate([gains[part] * w, wu[part, :, DK:]], axis=1)
        if starts[part] is not None:
            new = new - dot2(w, starts[part], NN)
        both = dot2(attend[part], new, NN)
        if starts[part] is not None:
            both = both + dot2(q_dec[part], starts[part], NN)
        coupling.append(gains[part] * q_dec[part] - both[:, :DK])
        base.append(both[:, DK:])
    coupling = jnp.concatenate(coupling, axis=0)
    base = jnp.concatenate(base, axis=0)

    sent = list(copies)
    for level in range(2):
        for copy in copies:
            copy.wait_recv()
        m, gain, before, before_gain = compose(level)
        if level == 0:
            copies = post(1, m, gain)
            sent += copies
        else:
            quarters = post_quarters(m, gain)
            sent += list(quarters.values())
        both = dot2(coupling, before, NN)
        coupling = before_gain * coupling - both[:, :DK]
        base = base + both[:, DK:]
    passed = []
    for turn in turns[2]:
        quarters[turn].wait_recv()
        place = board_2.at[(digits[2] + far - turn) % far, digits[0]]
        for side in turns[0]:
            passed.append(
                remote(place, 0, side, pass_sem.at[turn, side], got_sem.at[turn, side])
            )
    for copy in passed:
        copy.wait_recv()
    sent += passed

    def group(i):
        whole = board_2[i, :, pl.ds(0, SHARE), :].astype(F32).reshape(DK, 2 * DK)
        return whole, gain_of(board_2[i, 0, pl.ds(SHARE, EXTRA), :])

    def then(first, second):
        (m, gain), (m2, gain2) = first, second
        scaled = jnp.concatenate([gain[:, :DK] * m2[:, :DK], m2[:, DK:]], axis=1)
        return gain2 * m - dot2(m2[:, :DK], m, NN) + scaled, gain * gain2

    def step(state, element):
        m, gain = element
        return gain[:, :DK] * state - dot2(m[:, :DK], state, NN) + m[:, DK:]

    runs = {1: [group(i) for i in range(far)]}
    size = 1
    while 2 * size < far:
        runs[2 * size] = [
            then(runs[size][j], runs[size][j + 1]) if j else None
            for j in range(0, len(runs[size]), 2)
        ]
        size *= 2
    states = {1: runs[1][0][0][:, DK:]}
    size = 1
    while size < far:
        states[2 * size] = step(states[size], runs[size][1])
        size *= 2
    while size > 1:
        size //= 2
        for at in range(2 * size, far, 2 * size):
            states[at + size] = step(states[at], runs[size][at // size])
    state = states[far]
    entry = jnp.zeros((DK, DK), F32)
    for i in range(1, far):
        entry = jnp.where(digits[2] == i, states[i], entry)
    out = base + dot2(coupling, entry, NN)
    normed = out * lax.rsqrt(jnp.mean(out * out, axis=-1, keepdims=True) + EPS)
    mixed_ref[...] = (normed * gates[...]).astype(BF16)
    cache = state.astype(BF16)
    cache_ref[0] = cache
    probe = probe_ref[0].astype(F32)
    probe = probe * (lax.rsqrt(jnp.sum(probe * probe, axis=-1, keepdims=True) + EPS) * DK**-0.5)
    high, low = halves(jnp.broadcast_to(probe, (16, DK)))
    read_ref[0] = (dot(high, cache, NN) + dot(low, cache, NN))[0:1]
    rim_copy.wait_send()
    for copy in sent + passes + list(sends.values()):
        copy.wait_send()


def fused(x, wq, wk, wv, wz, wr, taps, speed, logs, gain, probe):
    rows = x.shape[0]
    depth = wq.shape[0]
    slots = depth // x.shape[1]
    parts = rows // ROWS
    any_space = pl.BlockSpec(memory_space=pl.ANY)
    vmem = pl.BlockSpec(memory_space=pltpu.VMEM)
    dma = pltpu.SemaphoreType.DMA
    block = pltpu.VMEM((parts, ROWS, DK), F32)
    return pl.pallas_call(
        kernel,
        out_shape=(
            jax.ShapeDtypeStruct((rows, DK), BF16),
            jax.ShapeDtypeStruct((1, DK, DK), BF16),
            jax.ShapeDtypeStruct((1, 1, DK), F32),
        ),
        in_specs=[any_space] * 11,
        out_specs=(vmem, vmem, vmem),
        scratch_shapes=[
            *[pltpu.VMEM(a.shape, a.dtype) for a in (taps, speed, logs, gain, probe)],
            pltpu.VMEM((slots, rows, depth // slots), BF16),
            pltpu.VMEM((slots, RIM, depth // slots), BF16),
            pltpu.VMEM((4, depth, DK), BF16),
            pltpu.VMEM(wr.shape, BF16),
            pltpu.VMEM((RIM, 3 * DK), BF16),
            pltpu.VMEM((RIM, 3 * DK), BF16),
            pltpu.VMEM((rows + RIM, 3 * DK), F32),
            pltpu.VMEM((rows, DK), F32),
            *[block] * 7,
            pltpu.VMEM((4, DK + EXTRA, 2 * DK), BF16),
            pltpu.VMEM((2, DK + EXTRA, 2 * DK), BF16),
            pltpu.VMEM((8, 4, SHARE + EXTRA, 2 * DK), BF16),
            dma((12,)),
            dma((parts + 1, 4)),
            dma((parts + 1, 4)),
            dma((parts + 1, 4)),
            dma((parts + 1, 4)),
            dma((2,)),
            dma((3, 8)),
            dma((3, 8)),
            dma((8, 4)),
            dma((8, 4)),
            pltpu.SemaphoreType.REGULAR((4,)),
        ],
        compiler_params=pltpu.CompilerParams(collective_id=0, has_side_effects=True),
    )(x, wq, wk, wv, wz, wr, taps, speed, logs, gain, probe)


def on_device(x, wq, wk, wv, wz, wr, taps, speed, logs, gain, probe):
    by_kind = wr.transpose(0, 2, 1).reshape(-1, wr.shape[1])
    return fused(
        x, wq, wk, wv, wz, by_kind, taps, speed.reshape(1, -1), logs.reshape(1, -1), gain.reshape(1, DK), probe
    )


def solution(mesh):
    in_specs = (
        P("sp", "tp"),
        P(None, "tp"),
        P(None, "tp"),
        P(None, "tp"),
        P(None, "tp"),
        P(),
        P(None, None, "tp"),
        P(),
        P("sp", "tp"),
        P(),
        P("sp", "tp", None),
    )
    out_specs = (P("sp", "tp"), P("tp", None, None), P("sp", "tp", None))
    return jax.shard_map(
        on_device, mesh=mesh, in_specs=in_specs, out_specs=out_specs, check_vma=False
    )
```

```python
import functools
import math

import jax
import jax.numpy as jnp
from jax import lax
from jax.experimental import pallas as pl
from jax.experimental.pallas import tpu as pltpu
from jax.sharding import PartitionSpec as P

DK = 128
CONV = 4
EPS = 1e-06
MESH = pl.DeviceIdType.MESH
F32 = jnp.float32
BF16 = jnp.bfloat16

ROWS = 128
RIM = 16
EXTRA = 8
TOKENS = True
SHARE = DK // 4


def silu(value):
    return value * jax.nn.sigmoid(value)


def halves(value):
    high = value.astype(BF16)
    low = (value - high.astype(F32)).astype(BF16)
    return high, low


def dot(left, right, dims):
    return lax.dot_general(left, right, dims, preferred_element_type=F32)


def dot3(left, right, dims):
    lh, ll = halves(left)
    rh, rl = halves(right)
    return dot(lh, rh, dims) + (dot(lh, rl, dims) + dot(ll, rh, dims))


def dot2(left, right, dims):
    lh, ll = halves(left)
    right = right.astype(BF16)
    left = jnp.concatenate([lh, ll], axis=-1)
    return dot(left, jnp.concatenate([right, right], axis=-2), dims)


NN = (((1,), (0,)), ((), ()))
NT = (((1,), (1,)), ((), ()))
TN = (((0,), (0,)), ((), ()))
BNN = (((2,), (1,)), ((0,), (0,)))
BNT = (((2,), (2,)), ((0,), (0,)))


def inverse_of_unit_lower(a, row, col):
    eye = (row == col).astype(F32)
    size = 8
    y = jnp.where(row // size == col // size, a, 0.0)
    t = eye - y
    y2 = dot3(y, y, BNN)
    t, y4 = t + dot3(t, y2, BNN), dot3(y2, y2, BNN)
    t = t + dot3(t, y4, BNN)
    while size < ROWS:
        joins = (row // (4 * size) == col // (4 * size)) & (row // size != col // size)
        n = dot2(t, jnp.where(joins, a, 0.0), BNN)
        t, n2 = t - dot2(n, t, BNN), dot2(n, n, BNN)
        t = t + dot2(n2, t, BNN)
        size *= 4
    return t


def kernel(
    x_hbm, wq_hbm, wk_hbm, wv_hbm, wz_hbm, wr_hbm,
    taps_hbm, speed_hbm, logs_hbm, gain_hbm, probe_hbm,
    mixed_ref, cache_ref, read_ref,
    taps_ref, speed_ref, logs_ref, gain_ref, probe_ref,
    x_all, x_tail, w_all, w_rate, tail, rim_in, ext, gates,
    q_ref, k_ref, kb_ref, vb_ref, a_ref, sum_ref, decay_ref,
    board_0, board_1, board_2,
    load_sem, near_send, near_recv, core_send, core_recv, rim_sem,
    send_sem, recv_sem, pass_sem, got_sem, token,
):
    sp = lax.axis_index("sp")
    tp = lax.axis_index("tp")
    n_sp = lax.axis_size("sp")
    chip, core = tp // 2, tp % 2
    partner = chip * 2 + (1 - core)
    rows, width = x_hbm.shape
    parts = rows // ROWS
    strides, counts = (1, 4, 8), (4, 2, n_sp // 8)
    far = counts[2]
    digits = [(sp // stride) % count for stride, count in zip(strides, counts)]
    turns = [
        (2, 1, 3),
        (1,),
        sorted(range(1, far), key=lambda turn: min(turn, far - turn)),
    ]

    def member(level, turn):
        digit = digits[level]
        return sp + ((digit + turn) % counts[level] - digit) * strides[level]

    def near(r):
        return ((chip + r) % 4) * 2 + core

    load_x = pltpu.make_async_copy(x_hbm, x_all.at[tp], load_sem.at[0])
    load_x.start()
    load_tail = pltpu.make_async_copy(
        x_hbm.at[pl.ds(rows - RIM, RIM), :], x_tail.at[tp], load_sem.at[6]
    )
    load_tail.start()
    after, before_sp = (sp + 1) % n_sp, (sp + n_sp - 1) % n_sp
    barrier = pltpu.get_barrier_semaphore()
    greeted = [(sp, near(r)) for r in (2, 1, 3)] + [(sp, partner), (after, tp), (before_sp, tp)]
    greeted += [(member(0, turn), tp) for turn in turns[0]] + [(member(1, 1), tp)]
    beyond = (1, far - 1) if TOKENS else turns[2]
    greeted += [(member(2, turn), tp) for turn in beyond]
    for peer in greeted:
        pl.semaphore_signal(barrier, inc=1, device_id=peer, device_id_type=MESH)
    loads = []
    for i, w in enumerate((wq_hbm, wk_hbm, wv_hbm, wz_hbm)):
        loads.append(
            pltpu.make_async_copy(w, w_all.at[i], load_sem.at[1 + i])
        )
    loads.append(pltpu.make_async_copy(wr_hbm, w_rate, load_sem.at[5]))
    small = (
        (taps_hbm, taps_ref), (speed_hbm, speed_ref), (logs_hbm, logs_ref),
        (gain_hbm, gain_ref), (probe_hbm, probe_ref),
    )
    for i, (source, place) in enumerate(small):
        loads.append(pltpu.make_async_copy(source, place, load_sem.at[7 + i]))
    for load in loads:
        load.start()

    load_x.wait()
    load_tail.wait()
    pl.semaphore_wait(barrier, len(greeted))

    def pass_token(i):
        if TOKENS and 0 < i < far // 2:
            pl.semaphore_wait(token.at[i - 1], 2)
        if TOKENS and i < far // 2 - 1:
            for turn in (1, far - 1):
                pl.semaphore_signal(
                    token.at[i], inc=1, device_id=(member(2, turn), tp), device_id_type=MESH
                )

    def block(part, slot):
        if part == parts:
            return x_tail.at[slot]
        return x_all.at[slot, pl.ds(part * ROWS, ROWS)]

    def to(place, peer, send, recv):
        copy = pltpu.make_async_remote_copy(
            src_ref=place, dst_ref=place, send_sem=send, recv_sem=recv,
            device_id=(sp, peer), device_id_type=MESH,
        )
        copy.start()
        return copy

    sends, passes = {}, []
    order = [parts] + list(range(parts))
    for part in order:
        for r in (2, 1, 3):
            sends[part, r] = to(
                block(part, tp), near(r), near_send.at[part, r], near_recv.at[part, r]
            )
        sends[part, 0] = to(
            block(part, tp), partner, core_send.at[part, 0], core_recv.at[part, 0]
        )
    pass_token(0)
    for load in loads:
        load.wait()

    def gathered(part):
        mine = []
        for r in (1, 3, 2):
            sends[part, r].wait_recv()
            slot = ((chip + 4 - r) % 4) * 2 + core
            mine.append(
                to(block(part, slot), partner, core_send.at[part, r], core_recv.at[part, r])
            )
        sends[part, 0].wait_recv()
        for copy in mine:
            copy.wait_recv()
        passes.extend(mine)

    gathered(parts)
    slots = x_all.shape[0]
    tail_x = jnp.concatenate([x_tail[slot] for slot in range(slots)], axis=1)
    three = jnp.concatenate([w_all[i] for i in range(3)], axis=1)
    tail[...] = dot(tail_x, three, NN).astype(BF16)
    rim_copy = pltpu.make_async_remote_copy(
        src_ref=tail, dst_ref=rim_in, send_sem=rim_sem.at[0], recv_sem=rim_sem.at[1],
        device_id=(after, tp), device_id_type=MESH,
    )
    rim_copy.start()
    pass_token(1)

    row = lax.broadcasted_iota(jnp.int32, (ROWS, ROWS), 0)
    col = lax.broadcasted_iota(jnp.int32, (ROWS, ROWS), 1)
    eye = (row == col).astype(F32)
    below = (row >= col).astype(BF16)
    gain_row = gain_ref[...].astype(F32)
    own_head = lax.broadcasted_iota(jnp.int32, speed_ref.shape, 1) == tp
    speed = jnp.sum(jnp.where(own_head, speed_ref[...], 0.0), axis=-1, keepdims=True)

    def prepare(part):
        here = pl.ds(part * ROWS, ROWS)
        x = jnp.concatenate([x_all[slot, here, :] for slot in range(slots)], axis=1)
        four = jnp.concatenate([w_all[i] for i in range(4)], axis=1)
        raw = dot(x, four, NN).astype(BF16).astype(F32)
        rates = dot(x, w_rate[...], NT)
        ext[pl.ds(RIM + part * ROWS, ROWS), :] = raw[:, : 3 * DK]
        gates[here, :] = silu(raw[:, 3 * DK :]) * gain_row
        outs = []
        for c in range(3):
            lanes = pl.ds(c * DK, DK)
            total = jnp.zeros((ROWS, DK), F32)
            for lag in range(CONV):
                tap = taps_ref[c, pl.ds(lag, 1), :].astype(F32)
                total = total + tap * ext[
                    pl.ds(part * ROWS + RIM - (CONV - 1) + lag, ROWS), lanes
                ]
            outs.append(silu(total))
        query, keys, values = outs
        query = query * (
            lax.rsqrt(jnp.sum(query * query, axis=-1, keepdims=True) + EPS) * DK**-0.5
        )
        keys = keys * lax.rsqrt(jnp.sum(keys * keys, axis=-1, keepdims=True) + EPS)
        kinds = rates.shape[1]
        kind = lax.broadcasted_iota(jnp.int32, (ROWS, kinds), 1)
        fade = jnp.sum(jnp.where(kind == tp, rates, 0.0), axis=-1, keepdims=True)
        write = jnp.sum(jnp.where(kind == tp + kinds // 2, rates, 0.0), axis=-1, keepdims=True)
        beta = jax.nn.sigmoid(write - math.log(4.0 * rows * n_sp / DK))
        soft = jnp.maximum(fade, 0.0) + jnp.log1p(jnp.exp(-jnp.abs(fade)))
        spread = jnp.broadcast_to(logs_ref[:, here], (ROWS, ROWS)).T - speed * soft
        high, low = halves(spread)
        lowest = (spread - high.astype(F32) - low.astype(F32)).astype(BF16)
        summed = dot(below, high, NN) + (dot(below, low, NN) + dot(below, lowest, NN))
        decay = jnp.exp(jnp.where(row >= col, summed - summed.T, -1e30))
        k_beta = keys * beta
        q_ref[part] = query
        k_ref[part] = keys
        kb_ref[part] = k_beta
        vb_ref[part] = values * beta
        sum_ref[part] = summed
        decay_ref[part] = decay
        a_ref[part] = jnp.where(row > col, dot3(k_beta, keys, NT) * decay, 0.0)

    for part in range(parts):
        gathered(part)
        if part == 0:
            rim_copy.wait_recv()
            ext[pl.ds(0, RIM), :] = jnp.where(sp == 0, 0.0, rim_in[...].astype(F32))
        prepare(part)
        pass_token(part + 2)

    query, keys, k_beta, summed, decay = (
        ref[...] for ref in (q_ref, k_ref, kb_ref, sum_ref, decay_ref)
    )
    t_mat = inverse_of_unit_lower(a_ref[...], row[None], col[None])
    grown = jnp.exp(summed)
    right = jnp.concatenate([k_beta * grown, vb_ref[...]], axis=2)
    wu = dot2(t_mat, right, BNN)
    k_dec = keys * jnp.exp(summed[:, ROWS - 1 :, :] - summed)
    last = grown[:, ROWS - 1 :, :]

    starts, gains = [], []
    m, gain = None, jnp.ones((1, DK), F32)
    for part in range(parts):
        step = dot3(k_dec[part], wu[part], TN)
        starts.append(m)
        gains.append(gain)
        if m is None:
            m = step
        else:
            twice = jnp.concatenate([last[part], last[part]], axis=1)
            scaled = jnp.concatenate([gain * step[:, :DK], step[:, DK:]], axis=1)
            m = twice * m - dot2(step[:, :DK], m, NN) + scaled
        gain = gain * last[part]

    def gain_rows(gain):
        g2 = jnp.concatenate([gain, gain], axis=1)
        high = g2.astype(BF16).astype(F32)
        mid = (g2 - high).astype(BF16).astype(F32)
        low = g2 - high - mid
        at = lax.broadcasted_iota(jnp.int32, (EXTRA, 2 * DK), 0)
        extra = jnp.where(at == 0, high, jnp.where(at == 1, mid, jnp.where(at == 2, low, 0.0)))
        return extra.astype(BF16)

    def gain_of(extra):
        extra = extra.astype(F32)
        return extra[0:1] + extra[1:2] + extra[2:3]

    boards = (board_0, board_1)

    def remote(place, level, turn, send, recv):
        copy = pltpu.make_async_remote_copy(
            src_ref=place, dst_ref=place, send_sem=send, recv_sem=recv,
            device_id=(member(level, turn), tp), device_id_type=MESH,
        )
        copy.start()
        return copy

    def post(level, m, gain):
        board, digit = boards[level], digits[level]
        board[digit, pl.ds(0, DK), :] = m.astype(BF16)
        board[digit, pl.ds(DK, EXTRA), :] = gain_rows(gain)
        return [
            remote(
                board.at[digit], level, turn,
                send_sem.at[level, turn], recv_sem.at[level, turn],
            )
            for turn in turns[level]
        ]

    def post_quarters(m, gain):
        rounded, extra = m.astype(BF16), gain_rows(gain)
        for i in range(4):
            board_2[digits[2], i, pl.ds(0, SHARE), :] = rounded[i * SHARE : (i + 1) * SHARE]
            board_2[digits[2], i, pl.ds(SHARE, EXTRA), :] = extra
        place = board_2.at[digits[2], digits[0]]
        return {
            turn: remote(place, 2, turn, send_sem.at[2, turn], recv_sem.at[2, turn])
            for turn in turns[2]
        }

    def read(level, i):
        board = boards[level]
        return board[i, pl.ds(0, DK), :].astype(F32), gain_of(board[i, pl.ds(DK, EXTRA), :])

    def then(first, second):
        (m, gain), (m2, gain2) = first, second
        scaled = jnp.concatenate([gain[:, :DK] * m2[:, :DK], m2[:, DK:]], axis=1)
        return gain2 * m - dot2(m2[:, :DK], m, NN) + scaled, gain * gain2

    def choose(level, before):
        m, gain = jnp.zeros((DK, 2 * DK), F32), jnp.ones((1, 2 * DK), F32)
        for i, (m_i, gain_i) in enumerate(before):
            m = jnp.where(digits[level] == i + 1, m_i, m)
            gain = jnp.where(digits[level] == i + 1, gain_i, gain)
        return m, gain[:, :DK]

    copies = post(0, m, gain)

    base, coupling = [], []
    attend = dot3(query, keys, BNT) * decay
    q_dec = query * grown
    for part in range(parts):
        w = wu[part, :, :DK]
        new = jnp.concatenate([gains[part] * w, wu[part, :, DK:]], axis=1)
        if starts[part] is not None:
            new = new - dot2(w, starts[part], NN)
        both = dot2(attend[part], new, NN)
        if starts[part] is not None:
            both = both + dot2(q_dec[part], starts[part], NN)
        coupling.append(gains[part] * q_dec[part] - both[:, :DK])
        base.append(both[:, DK:])
    coupling = jnp.concatenate(coupling, axis=0)
    base = jnp.concatenate(base, axis=0)

    sent = list(copies)
    for level in range(2):
        for copy in copies:
            copy.wait_recv()
        members = [read(level, i) for i in range(counts[level])]
        left = then(members[0], members[1])
        if level == 0:
            m, gain = then(left, then(members[2], members[3]))
            copies = post(1, m, gain[:, :DK])
            sent += copies
            known = [members[0], left, then(left, members[2])]
        else:
            m, gain = left
            quarters = post_quarters(m, gain[:, :DK])
            sent += list(quarters.values())
            known = [members[0]]
        before, before_gain = choose(level, known)
        both = dot2(coupling, before, NN)
        coupling = before_gain * coupling - both[:, :DK]
        base = base + both[:, DK:]
    passed = []
    for turn in turns[2]:
        quarters[turn].wait_recv()
        place = board_2.at[(digits[2] + far - turn) % far, digits[0], pl.ds(0, SHARE), :]
        for side in turns[0]:
            passed.append(
                remote(place, 0, side, pass_sem.at[turn, side], got_sem.at[turn, side])
            )
    for copy in passed:
        copy.wait_recv()
    sent += passed

    def group(i):
        whole = board_2[i, :, pl.ds(0, SHARE), :].astype(F32).reshape(DK, 2 * DK)
        return whole, gain_of(board_2[i, digits[0], pl.ds(SHARE, EXTRA), :])

    def step(state, element):
        m, gain = element
        return gain[:, :DK] * state - dot2(m[:, :DK], state, NN) + m[:, DK:]

    runs = {1: [group(i) for i in range(far)]}
    size = 1
    while 2 * size < far:
        runs[2 * size] = [
            then(runs[size][j], runs[size][j + 1]) if j else None
            for j in range(0, len(runs[size]), 2)
        ]
        size *= 2
    states = {1: runs[1][0][0][:, DK:]}
    size = 1
    while size < far:
        states[2 * size] = step(states[size], runs[size][1])
        size *= 2
    while size > 1:
        size //= 2
        for at in range(2 * size, far, 2 * size):
            states[at + size] = step(states[at], runs[size][at // size])
    state = states[far]
    entry = jnp.zeros((DK, DK), F32)
    for i in range(1, far):
        entry = jnp.where(digits[2] == i, states[i], entry)
    out = base + dot2(coupling, entry, NN)
    normed = out * lax.rsqrt(jnp.mean(out * out, axis=-1, keepdims=True) + EPS)
    mixed_ref[...] = (normed * gates[...]).astype(BF16)
    cache = state.astype(BF16)
    cache_ref[0] = cache
    probe = probe_ref[0].astype(F32)
    probe = probe * (lax.rsqrt(jnp.sum(probe * probe, axis=-1, keepdims=True) + EPS) * DK**-0.5)
    high, low = halves(jnp.broadcast_to(probe, (16, DK)))
    read_ref[0] = (dot(high, cache, NN) + dot(low, cache, NN))[0:1]
    rim_copy.wait_send()
    for copy in sent + passes + list(sends.values()):
        copy.wait_send()


def fused(x, wq, wk, wv, wz, wr, taps, speed, logs, gain, probe):
    rows = x.shape[0]
    depth = wq.shape[0]
    slots = depth // x.shape[1]
    parts = rows // ROWS
    any_space = pl.BlockSpec(memory_space=pl.ANY)
    vmem = pl.BlockSpec(memory_space=pltpu.VMEM)
    dma = pltpu.SemaphoreType.DMA
    block = pltpu.VMEM((parts, ROWS, DK), F32)
    return pl.pallas_call(
        kernel,
        out_shape=(
            jax.ShapeDtypeStruct((rows, DK), BF16),
            jax.ShapeDtypeStruct((1, DK, DK), BF16),
            jax.ShapeDtypeStruct((1, 1, DK), F32),
        ),
        in_specs=[any_space] * 11,
        out_specs=(vmem, vmem, vmem),
        scratch_shapes=[
            *[pltpu.VMEM(a.shape, a.dtype) for a in (taps, speed, logs, gain, probe)],
            pltpu.VMEM((slots, rows, depth // slots), BF16),
            pltpu.VMEM((slots, RIM, depth // slots), BF16),
            pltpu.VMEM((4, depth, DK), BF16),
            pltpu.VMEM(wr.shape, BF16),
            pltpu.VMEM((RIM, 3 * DK), BF16),
            pltpu.VMEM((RIM, 3 * DK), BF16),
            pltpu.VMEM((rows + RIM, 3 * DK), F32),
            pltpu.VMEM((rows, DK), F32),
            *[block] * 7,
            pltpu.VMEM((4, DK + EXTRA, 2 * DK), BF16),
            pltpu.VMEM((2, DK + EXTRA, 2 * DK), BF16),
            pltpu.VMEM((8, 4, SHARE + EXTRA, 2 * DK), BF16),
            dma((12,)),
            dma((parts + 1, 4)),
            dma((parts + 1, 4)),
            dma((parts + 1, 4)),
            dma((parts + 1, 4)),
            dma((2,)),
            dma((3, 8)),
            dma((3, 8)),
            dma((8, 4)),
            dma((8, 4)),
            pltpu.SemaphoreType.REGULAR((4,)),
        ],
        compiler_params=pltpu.CompilerParams(collective_id=0, has_side_effects=True),
    )(x, wq, wk, wv, wz, wr, taps, speed, logs, gain, probe)


def placed_kernel(mixed, cache, read, mixed_out, cache_out, read_out):
    mixed_out[...] = mixed[...]
    cache_out[...] = cache[...]
    read_out[...] = read[...]


def placed(outs):
    vmem = pl.BlockSpec(memory_space=pltpu.VMEM)
    return pl.pallas_call(
        placed_kernel,
        out_shape=tuple(jax.ShapeDtypeStruct(out.shape, out.dtype) for out in outs),
        in_specs=[vmem] * 3,
        out_specs=(vmem,) * 3,
    )(*outs)


def on_device(x, wq, wk, wv, wz, wr, taps, speed, logs, gain, probe):
    by_kind = wr.transpose(0, 2, 1).reshape(-1, wr.shape[1])
    outs = fused(
        x, wq, wk, wv, wz, by_kind, taps, speed.reshape(1, -1), logs.reshape(1, -1), gain.reshape(1, DK), probe
    )
    return placed(outs)


def solution(mesh):
    in_specs = (
        P("sp", "tp"),
        P(None, "tp"),
        P(None, "tp"),
        P(None, "tp"),
        P(None, "tp"),
        P(),
        P(None, None, "tp"),
        P(),
        P("sp", "tp"),
        P(),
        P("sp", "tp", None),
    )
    out_specs = (P("sp", "tp"), P("tp", None, None), P("sp", "tp", None))
    return jax.shard_map(
        on_device, mesh=mesh, in_specs=in_specs, out_specs=out_specs, check_vma=False
    )
```
